32 devices in a mesh: sp: 8 (over z, x), dp: 4 (over y, core).
Axes of the slice: x: 2, y: 2, z: 4, core: 2. Of those that a mesh axis runs over, the one named last changes fastest.
Arguments:
- lin_pre: bfloat16 [2048, 8192], P(None, ('dp', 'sp')), may hold values from -6 to 6
- gate_pre: bfloat16 [2048, 8192], P(None, ('dp', 'sp')), may hold values from -8 to 8
- w_depth: float32 [31, 2048], replicated, may hold values from -1 to 1
- ln_gain: float32 [2048], replicated, may hold values from 0.1 to 1.9
- ln_shift: float32 [2048], replicated, may hold values from -3 to 3
- w_out: bfloat16 [2048, 2048], P(None, 'dp'), may hold values from -0.125 to 0.125
Outputs:
- module_out: bfloat16 [8192, 2048], P(('dp', 'sp'))
The draws below stay inside these ranges and needn't reach their ends.
All inputs are finite; a program needn't handle non-finite values.
Results may differ from the reference program's by a relative error of at most 0.0064.
Values may be sent and summed in bfloat16 or wider, within the bound.
A program may use at most 64 MiB of HBM per device.

```python
import jax
import jax.numpy as jnp
from jax import lax

D = 2048
KERNEL = 31
HALF = 15
LENGTH = 2048
TOKENS = 8192
N_DP = 4


def shard_levels(key, dims, split, low, top_value):
    gain = 1.0
    for axis_at, shards_of in split:
        steps = jax.random.uniform(jax.random.fold_in(jax.random.fold_in(key, 6), axis_at), (shards_of,), jnp.float32, low / len(split), top_value / len(split))
        gain = gain * jnp.repeat(jnp.exp(steps), dims[axis_at] // shards_of).reshape((-1,) + (1,) * (len(dims) - 1 - axis_at))
    return gain


def bell_draw(rng, dims, width, reach, pieces=(), dtype=jnp.bfloat16):
    values = width * jax.random.normal(rng, dims, jnp.float32)
    if pieces:
        values = values * shard_levels(rng, dims, pieces, -0.22, 0.18)
    return jnp.clip(values, -reach, reach).astype(dtype)


def setup_inputs(seed: int = 0) -> dict:
    seeds = jax.random.split(jax.random.key(seed), 7)
    lin_pre = bell_draw(seeds[0], (D, TOKENS), 1.0, 6.0, ((1, 32),))
    gate_pre = bell_draw(seeds[1], (D, TOKENS), 1.5, 8.0, ((1, 32),))
    w_depth = bell_draw(seeds[2], (KERNEL, D), KERNEL ** -0.5, 1.0, (), jnp.float32)
    ln_gain = jnp.clip(1.0 + 0.18 * jax.random.normal(seeds[3], (D,), jnp.float32), 0.1, 1.9)
    ln_shift = bell_draw(seeds[4], (D,), 0.5, 3.0, (), jnp.float32)
    w_out = bell_draw(seeds[5], (D, D), D ** -0.5, 0.125, ((1, 4),))
    return dict(lin_pre=lin_pre, gate_pre=gate_pre, w_depth=w_depth, ln_gain=ln_gain, ln_shift=ln_shift, w_out=w_out)


def one_sequence(glu_seq, w_depth, ln_gain, ln_shift, w_out):
    padded = jnp.pad(glu_seq.astype(jnp.float32), ((0, 0), (HALF, HALF)))
    running = jnp.zeros(glu_seq.shape, jnp.float32)
    for tap_index in range(KERNEL):
        running = running + w_depth[tap_index][:, None] * padded[:, tap_index:tap_index + LENGTH]
    mixed = running.astype(jnp.bfloat16)
    mixed_float = mixed.astype(jnp.float32)
    channel_mean = lax.optimization_barrier(jnp.mean(mixed_float, axis=0, keepdims=True))
    variance = lax.optimization_barrier(jnp.mean(jnp.square(mixed_float - channel_mean), axis=0, keepdims=True))
    normed = (mixed_float - channel_mean) * lax.rsqrt(variance + 1e-05)
    normed = normed * ln_gain[:, None] + ln_shift[:, None]
    activated = jax.nn.silu(normed).astype(jnp.bfloat16)
    projected = lax.dot_general(activated, w_out, (((0,), (0,)), ((), ())), preferred_element_type=jnp.float32)
    return projected.astype(jnp.bfloat16)

def reference(lin_pre, gate_pre, w_depth, ln_gain, ln_shift, w_out):
    glu = (lin_pre.astype(jnp.float32) * jax.nn.sigmoid(gate_pre.astype(jnp.float32))).astype(jnp.bfloat16)
    stacked = glu.reshape(D, N_DP, LENGTH).transpose(1, 0, 2)
    result = lax.map(lambda glu_seq: one_sequence(glu_seq, w_depth, ln_gain, ln_shift, w_out), stacked)
    return result.reshape(TOKENS, D)
```

```python
import functools

import jax
import jax.numpy as jnp
from jax import lax
from jax.experimental import pallas as pl
from jax.experimental.pallas import tpu as pltpu
from jax.sharding import PartitionSpec as P

MESH = pl.DeviceIdType.MESH
LANES = 128
PAD = 16
CHUNKS = 4


def kernel(
    n_sp, n_dp, lin_hbm, gate_hbm, taps, gain, shift, w_hbm, out,
    lin_v, gate_v, gpad, mixed, act, wbuf, stat,
    in_sem, own_sem, own_d2d, halo_send, halo_recv,
    y_send, y_recv, x_send, x_recv, z_send, z_recv, d_send, d_recv,
):
    channels, span = lin_hbm.shape
    taps_n = taps.shape[0]
    half = (taps_n - 1) // 2
    width = w_hbm.shape[1]
    slabs = channels // LANES
    s = lax.axis_index("sp")
    d = lax.axis_index("dp")
    g, core = d // 2, d % 2
    groups = n_dp // 2
    partner = (s, g * 2 + 1 - core)
    flip1 = s + 1 - 2 * (s % 2)
    hi = (s // 2) % 2
    flip2 = s + 2 - 4 * hi
    q = s % 4
    q1 = q + 1 - 2 * (s % 2)
    q2 = q + 2 - 4 * hi
    q3 = 3 - q
    piece = channels // 4
    rows = piece // CHUNKS
    n_b = CHUNKS // 4

    in_rows = channels // 4
    loads = []
    for i in range(4):
        for a, (src, dst) in enumerate(((gate_hbm, gate_v), (lin_hbm, lin_v))):
            cut = pl.ds(i * in_rows, in_rows)
            loads.append(pltpu.make_async_copy(src.at[cut, :], dst.at[cut, :], in_sem.at[a, i]))
            loads[-1].start()

    barrier = pltpu.get_barrier_semaphore()
    peers = [partner, (flip1, d), (flip2, d)]
    for k in range(1, groups):
        peers.append((s, ((g + k) % groups) * 2 + core))
    peers += [(lax.rem(s + 1, n_sp), d), (lax.rem(s + n_sp - 1, n_sp), d)]
    for peer in peers:
        pl.semaphore_signal(barrier, inc=1, device_id=peer, device_id_type=MESH)
    pl.semaphore_wait(barrier, len(peers))
    has_left, has_right = s > 0, s < n_sp - 1

    sends = []

    def at(block, p, i):
        start = pl.multiple_of(p * piece + i * rows, rows)
        return wbuf.at[block, pl.ds(start, rows), :]

    def own(p, i):
        start = pl.multiple_of(p * piece + i * rows, rows)
        return w_hbm.at[pl.ds(start, rows), :]

    def copy(src, dst, send, recv, device):
        return pltpu.make_async_remote_copy(
            src_ref=src, dst_ref=dst, send_sem=send, recv_sem=recv,
            device_id=device, device_id_type=MESH,
        )

    def push(*args):
        c = copy(*args)
        c.start()
        sends.append(c)

    n_a = CHUNKS - 2 * n_b
    b_part = list(range(0, n_b))
    c_part = list(range(n_b, 2 * n_b))
    a_part = list(range(2 * n_b, CHUNKS))
    for k in range(1, groups):
        target = (s, ((g + k) % groups) * 2 + core)
        for i in range(CHUNKS):
            push(own(q, i), at(d, q, i), y_send.at[k - 1, i], y_recv.at[k - 1, i], target)
        for n, i in enumerate(a_part):
            m = CHUNKS + n
            push(own(q3, i), at(d, q3, i), y_send.at[k - 1, m], y_recv.at[k - 1, m], target)
    push(w_hbm, wbuf.at[d], own_d2d.at[0], own_d2d.at[1], partner)
    own_copy = pltpu.make_async_copy(w_hbm, wbuf.at[d], own_sem)
    own_copy.start()

    def landed(block, p, i, send, recv):
        ref = at(block, p, i)
        copy(ref, ref, send, recv, partner).wait_recv()
        return ref

    def to_partner(ref, k, m):
        push(ref, ref, d_send.at[k - 1, m], d_recv.at[k - 1, m], partner)

    events = []

    def event(kind, k, i):
        def run():
            block = ((g + groups - k) % groups) * 2 + core
            if kind == "y":
                ref = landed(block, q, i, y_send.at[k - 1, i], y_recv.at[k - 1, i])
                push(ref, ref, x_send.at[k - 1, i], x_recv.at[k - 1, i], (flip1, d))
                push(ref, ref, z_send.at[k - 1, i], z_recv.at[k - 1, i], (flip2, d))
                to_partner(ref, k, i)
            elif kind == "x":
                ref = landed(block, q1, i, x_send.at[k - 1, i], x_recv.at[k - 1, i])
                if i in c_part:
                    m = CHUNKS + i - n_b
                    push(ref, ref, z_send.at[k - 1, m], z_recv.at[k - 1, m], (flip2, d))
                to_partner(ref, k, CHUNKS + i)
            elif kind == "z":
                ref = landed(block, q2, i, z_send.at[k - 1, i], z_recv.at[k - 1, i])
                if i in b_part:
                    m = CHUNKS + i
                    push(ref, ref, x_send.at[k - 1, m], x_recv.at[k - 1, m], (flip1, d))
                to_partner(ref, k, 2 * CHUNKS + i)
            elif kind == "yd":
                m = CHUNKS + i - 2 * n_b
                ref = landed(block, q3, i, y_send.at[k - 1, m], y_recv.at[k - 1, m])
                to_partner(ref, k, 3 * CHUNKS + i)
            elif kind == "xd":
                m = CHUNKS + i
                ref = landed(block, q3, i, x_send.at[k - 1, m], x_recv.at[k - 1, m])
                to_partner(ref, k, 3 * CHUNKS + i)
            else:
                m = CHUNKS + i - n_b
                ref = landed(block, q3, i, z_send.at[k - 1, m], z_recv.at[k - 1, m])
                to_partner(ref, k, 3 * CHUNKS + i)

        return run

    for k in range(1, groups):
        for i in range(CHUNKS + 1):
            if i < CHUNKS:
                events.append(event("y", k, i))
            if i > 0:
                events.append(event("x", k, i - 1))
                events.append(event("z", k, i - 1))
        for i in a_part[:-1]:
            events.append(event("yd", k, i))
        for i in b_part:
            events.append(event("xd", k, i))
        for i in c_part:
            events.append(event("zd", k, i))
        for i in a_part[-1:]:
            events.append(event("yd", k, i))

    def advance(count):
        for _ in range(min(count, len(events))):
            events.pop(0)()

    step = 2 * LANES
    eye = (
        lax.broadcasted_iota(jnp.int32, (span, span), 0)
        == lax.broadcasted_iota(jnp.int32, (span, span), 1)
    ).astype(jnp.float32).astype(jnp.bfloat16)

    @pl.when(jnp.logical_not(has_left))
    def _():
        gpad[:, 0:PAD, :] = jnp.zeros((slabs, PAD, LANES), jnp.float32)

    @pl.when(jnp.logical_not(has_right))
    def _():
        gpad[:, PAD + span :, :] = jnp.zeros((slabs, PAD, LANES), jnp.float32)

    for i in range(4):
        loads[2 * i].wait()
        loads[2 * i + 1].wait()
        per = in_rows // step

        def turn(n, carry):
            at_row = pl.multiple_of(n * step, step)
            cut = pl.ds(at_row, step)
            glu = (
                lin_v[cut, :].astype(jnp.float32)
                * jax.nn.sigmoid(gate_v[cut, :].astype(jnp.float32))
            ).astype(jnp.bfloat16)
            turned = lax.dot_general(
                eye, glu, (((1,), (1,)), ((), ())), preferred_element_type=jnp.float32
            )
            gpad[2 * n, pl.ds(PAD, span), :] = turned[:, :LANES]
            gpad[2 * n + 1, pl.ds(PAD, span), :] = turned[:, LANES:]
            return carry

        lax.fori_loop(i * per, (i + 1) * per, turn, 0)

    to_left = copy(
        gpad.at[:, pl.ds(PAD, PAD), :], gpad.at[:, pl.ds(PAD + span, PAD), :],
        halo_send.at[0], halo_recv.at[0], (s - 1, d),
    )
    to_right = copy(
        gpad.at[:, pl.ds(span, PAD), :], gpad.at[:, pl.ds(0, PAD), :],
        halo_send.at[1], halo_recv.at[1], (s + 1, d),
    )

    @pl.when(has_left)
    def _():
        to_left.start()

    @pl.when(has_right)
    def _():
        to_right.start()

    advance(1)

    @pl.when(has_left)
    def _():
        to_right.wait_recv()

    @pl.when(has_right)
    def _():
        to_left.wait_recv()

    tile = min(LANES, span)
    stat[0] = jnp.zeros((span, LANES), jnp.float32)

    def conv_slab(n, carry):
        lanes = pl.ds(pl.multiple_of(n * LANES, LANES), LANES)

        def tokens(t, inner):
            base = t * tile
            running = jnp.zeros((tile, LANES), jnp.float32)
            for j in range(taps_n):
                weight = taps[pl.ds(j, 1), lanes]
                running = running + weight * gpad[n, pl.ds(base + (PAD - half + j), tile), :]
            rounded = running.astype(jnp.bfloat16).astype(jnp.float32)
            at_token = pl.ds(pl.multiple_of(base, tile), tile)
            mixed[n, at_token, :] = rounded
            stat[0, at_token, :] += rounded
            return inner

        return lax.fori_loop(0, span // tile, tokens, carry)

    parts = 8
    for i in range(parts):
        lax.fori_loop(i * slabs // parts, (i + 1) * slabs // parts, conv_slab, 0)
        advance(2)

    mean = jnp.sum(stat[0], axis=1, keepdims=True) * (1.0 / channels)
    stat[0] = jnp.broadcast_to(mean, (span, LANES))
    stat[1] = jnp.zeros((span, LANES), jnp.float32)

    def spread(n, carry):
        apart = mixed[n] - stat[0]
        stat[1] += apart * apart
        return carry

    lax.fori_loop(0, slabs, spread, 0)
    variance = jnp.sum(stat[1], axis=1, keepdims=True) * (1.0 / channels)
    stat[1] = jnp.broadcast_to(lax.rsqrt(variance + 1e-05), (span, LANES))

    def activate(n, carry):
        lanes = pl.ds(pl.multiple_of(n * LANES, LANES), LANES)
        normed = (mixed[n] - stat[0]) * stat[1]
        normed = normed * gain[:, lanes] + shift[:, lanes]
        act[:, lanes] = (normed * jax.nn.sigmoid(normed)).astype(jnp.bfloat16)
        return carry

    lax.fori_loop(0, slabs, activate, 0)

    cols = min(width, 2 * LANES)

    def product(block):
        def columns(n, carry):
            at_col = pl.ds(pl.multiple_of(n * cols, cols), cols)
            at_out = pl.ds(pl.multiple_of(block * width + n * cols, cols), cols)
            out[:, at_out] = jnp.dot(
                act[...], wbuf[block, :, at_col], preferred_element_type=jnp.float32
            ).astype(out.dtype)
            return carry

        lax.fori_loop(0, width // cols, columns, 0)

    own_copy.wait()
    product(d)
    other = g * 2 + 1 - core
    copy(wbuf.at[other], wbuf.at[other], own_d2d.at[0], own_d2d.at[1], partner).wait_recv()
    product(other)
    advance(len(events))
    for k in range(1, groups):
        product(((g + groups - k) % groups) * 2 + core)
    for k in range(1, groups):
        block = ((g + groups - k) % groups) * 2 + 1 - core
        for p, at_piece in enumerate((q, q1, q2, q3)):
            for i in range(CHUNKS):
                m = p * CHUNKS + i
                landed(block, at_piece, i, d_send.at[k - 1, m], d_recv.at[k - 1, m])
        product(block)

    for c in sends:
        c.wait_send()

    @pl.when(has_left)
    def _():
        to_left.wait_send()

    @pl.when(has_right)
    def _():
        to_right.wait_send()


def solution(mesh):
    n_sp, n_dp = mesh.shape["sp"], mesh.shape["dp"]

    def per_device(lin_pre, gate_pre, w_depth, ln_gain, ln_shift, w_out):
        channels, span = lin_pre.shape
        width = w_out.shape[1]
        far = n_dp // 2 - 1
        n_b = CHUNKS // 4
        n_a = CHUNKS - 2 * n_b
        slabs = channels // LANES
        dma = pltpu.SemaphoreType.DMA
        vmem = pl.BlockSpec(memory_space=pltpu.VMEM)
        hbm = pl.BlockSpec(memory_space=pl.ANY)
        return pl.pallas_call(
            functools.partial(kernel, n_sp, n_dp),
            out_shape=jax.ShapeDtypeStruct((span, n_dp * width), jnp.bfloat16),
            in_specs=[hbm, hbm, vmem, vmem, vmem, hbm],
            out_specs=vmem,
            scratch_shapes=[
                pltpu.VMEM((channels, span), jnp.bfloat16),
                pltpu.VMEM((channels, span), jnp.bfloat16),
                pltpu.VMEM((slabs, span + 2 * PAD, LANES), jnp.float32),
                pltpu.VMEM((slabs, span, LANES), jnp.float32),
                pltpu.VMEM((span, channels), jnp.bfloat16),
                pltpu.VMEM((n_dp, channels, width), jnp.bfloat16),
                pltpu.VMEM((2, span, LANES), jnp.float32),
                dma((2, 4)),
                dma,
                dma((2,)),
                dma((2,)),
                dma((2,)),
                dma((far, CHUNKS + n_a)),
                dma((far, CHUNKS + n_a)),
                dma((far, CHUNKS + n_b)),
                dma((far, CHUNKS + n_b)),
                dma((far, CHUNKS + n_b)),
                dma((far, CHUNKS + n_b)),
                dma((far, 4 * CHUNKS)),
                dma((far, 4 * CHUNKS)),
            ],
            compiler_params=pltpu.CompilerParams(
                collective_id=0, has_side_effects=True, vmem_limit_bytes=60 * 2**20
            ),
            name="conv_module",
        )(lin_pre, gate_pre, w_depth, ln_gain[None, :], ln_shift[None, :], w_out)

    in_specs = (P(None, ("dp", "sp")), P(None, ("dp", "sp")), P(), P(), P(), P(None, "dp"))
    out_specs = P(("dp", "sp"), None)
    return jax.shard_map(
        per_device, mesh=mesh, in_specs=in_specs, out_specs=out_specs, check_vma=False
    )
```

```python
import functools

import jax
import jax.numpy as jnp
from jax import lax
from jax.experimental import pallas as pl
from jax.experimental.pallas import tpu as pltpu
from jax.sharding import PartitionSpec as P

MESH = pl.DeviceIdType.MESH
LANES = 128
PAD = 16
CHUNKS = 8
BY_X = 1
BY_Z = 2
BY_Y = CHUNKS - BY_X - BY_Z


def kernel(
    n_sp, n_dp, lin_hbm, gate_hbm, taps_hbm, gain_hbm, shift_hbm, w_hbm, out,
    lin_v, gate_v, taps, gain, shift, gpad, mixed, act, wbuf, stat, part, edge_out, edge_in,
    in_sem, small_sem, own_sem, own_d2d, halo_send, halo_recv,
    y_send, y_recv, x_send, x_recv, z_send, z_recv, d_send, d_recv,
):
    channels, span = lin_hbm.shape
    taps_n = taps.shape[0]
    half = (taps_n - 1) // 2
    width = w_hbm.shape[1]
    slabs = channels // LANES
    s = lax.axis_index("sp")
    d = lax.axis_index("dp")
    g, core = d // 2, d % 2
    groups = n_dp // 2
    partner = (s, g * 2 + 1 - core)
    other = g * 2 + 1 - core
    hi = (s // 2) % 2
    flip1 = s + 1 - 2 * (s % 2)
    flip2 = s + 2 - 4 * hi
    q = s % 4
    q1 = q + 1 - 2 * (s % 2)
    q2 = q + 2 - 4 * hi
    q3 = 3 - q
    piece = channels // 4
    rows = piece // CHUNKS

    barrier = pltpu.get_barrier_semaphore()
    peers = [partner, (flip1, d), (flip2, d)]
    for k in range(1, groups):
        peers.append((s, ((g + k) % groups) * 2 + core))
    peers += [(lax.rem(s + 1, n_sp), d), (lax.rem(s + n_sp - 1, n_sp), d)]
    for peer in peers:
        pl.semaphore_signal(barrier, inc=1, device_id=peer, device_id_type=MESH)
    has_left, has_right = s > 0, s < n_sp - 1

    def load(src, dst, sem):
        c = pltpu.make_async_copy(src, dst, sem)
        c.start()
        return c

    def piece_of(p):
        return pl.ds(pl.multiple_of(p * piece, piece), piece)

    def own_piece(n, p):
        return load(w_hbm.at[piece_of(p), :], wbuf.at[d, piece_of(p), :], own_sem.at[n])

    own_loads = [own_piece(0, q)]
    in_rows = channels // 4
    loads = []
    for i in range(4):
        cut = pl.ds(i * in_rows, in_rows)
        loads.append(load(gate_hbm.at[cut, :], gate_v.at[cut, :], in_sem.at[0, i]))
        loads.append(load(lin_hbm.at[cut, :], lin_v.at[cut, :], in_sem.at[1, i]))
    own_loads.append(own_piece(1, q3))
    small = [
        load(src, dst, small_sem.at[n])
        for n, (src, dst) in enumerate(((taps_hbm, taps), (gain_hbm, gain), (shift_hbm, shift)))
    ]
    own_loads.append(own_piece(2, q1))
    own_loads.append(own_piece(3, q2))

    sends = []

    def at(block, p, i):
        start = pl.multiple_of(p * piece + i * rows, rows)
        return wbuf.at[block, pl.ds(start, rows), :]

    def copy(src, dst, send, recv, device):
        return pltpu.make_async_remote_copy(
            src_ref=src, dst_ref=dst, send_sem=send, recv_sem=recv,
            device_id=device, device_id_type=MESH,
        )

    def push(*args):
        c = copy(*args)
        c.start()
        sends.append(c)

    own_loads[0].wait()
    pl.semaphore_wait(barrier, len(peers))

    b_part = list(range(0, BY_X))
    c_part = list(range(BY_X, BY_X + BY_Z))
    a_part = list(range(BY_X + BY_Z, CHUNKS))

    def send_y(p, i, m):
        for k in range(1, groups):
            target = (s, ((g + k) % groups) * 2 + core)
            push(at(d, p, i), at(d, p, i), y_send.at[k - 1, m], y_recv.at[k - 1, m], target)

    for i in range(CHUNKS):
        send_y(q, i, i)
    own_loads[1].wait()
    for n, i in enumerate(a_part):
        send_y(q3, i, CHUNKS + n)

    def landed(block, p, i, send, recv):
        ref = at(block, p, i)
        copy(ref, ref, send, recv, partner).wait_recv()
        return ref

    def to_partner(ref, k, m):
        push(ref, ref, d_send.at[k - 1, m], d_recv.at[k - 1, m], partner)

    def event(kind, k, i):
        def run():
            block = ((g + groups - k) % groups) * 2 + core
            if kind == "y":
                ref = landed(block, q, i, y_send.at[k - 1, i], y_recv.at[k - 1, i])
                push(ref, ref, x_send.at[k - 1, i], x_recv.at[k - 1, i], (flip1, d))
                push(ref, ref, z_send.at[k - 1, i], z_recv.at[k - 1, i], (flip2, d))
                to_partner(ref, k, i)
            elif kind == "x":
                ref = landed(block, q1, i, x_send.at[k - 1, i], x_recv.at[k - 1, i])
                if i in c_part:
                    m = CHUNKS + i - BY_X
                    push(ref, ref, z_send.at[k - 1, m], z_recv.at[k - 1, m], (flip2, d))
                to_partner(ref, k, CHUNKS + i)
            elif kind == "z":
                ref = landed(block, q2, i, z_send.at[k - 1, i], z_recv.at[k - 1, i])
                if i in b_part:
                    m = CHUNKS + i
                    push(ref, ref, x_send.at[k - 1, m], x_recv.at[k - 1, m], (flip1, d))
                to_partner(ref, k, 2 * CHUNKS + i)
            elif kind == "yd":
                m = CHUNKS + i - BY_X - BY_Z
                ref = landed(block, q3, i, y_send.at[k - 1, m], y_recv.at[k - 1, m])
                to_partner(ref, k, 3 * CHUNKS + i)
            elif kind == "xd":
                m = CHUNKS + i
                ref = landed(block, q3, i, x_send.at[k - 1, m], x_recv.at[k - 1, m])
                to_partner(ref, k, 3 * CHUNKS + i)
            else:
                m = CHUNKS + i - BY_X
                ref = landed(block, q3, i, z_send.at[k - 1, m], z_recv.at[k - 1, m])
                to_partner(ref, k, 3 * CHUNKS + i)

        return run

    plan = []
    for k in range(1, groups):
        for i in range(CHUNKS):
            plan.append((i + 1.0, event("y", k, i)))
            plan.append((i + 4.0, event("z", k, i)))
            plan.append((i + 4.5, event("x", k, i)))
        for n, i in enumerate(a_part):
            plan.append((CHUNKS + 1.0 + n, event("yd", k, i)))
        for n, i in enumerate(c_part):
            plan.append((CHUNKS + 4.0 + n, event("zd", k, i)))
        for n, i in enumerate(b_part):
            plan.append((CHUNKS + 4.5 + n, event("xd", k, i)))

    step = 2 * LANES
    eye = (
        lax.broadcasted_iota(jnp.int32, (span, span), 0)
        == lax.broadcasted_iota(jnp.int32, (span, span), 1)
    ).astype(jnp.float32).astype(jnp.bfloat16)

    for i in range(4):
        loads[2 * i].wait()
        loads[2 * i + 1].wait()
        per = in_rows // step

        def turn(n, carry):
            at_row = pl.multiple_of(n * step, step)
            cut = pl.ds(at_row, step)
            glu = (
                lin_v[cut, :].astype(jnp.float32)
                * jax.nn.sigmoid(gate_v[cut, :].astype(jnp.float32))
            ).astype(jnp.bfloat16)
            turned = lax.dot_general(
                eye, glu, (((1,), (1,)), ((), ())), preferred_element_type=jnp.float32
            )
            for m in range(2):
                slab = turned[:, m * LANES : (m + 1) * LANES]
                gpad[2 * n + m, pl.ds(PAD, span), :] = slab
                edge_out[0, 2 * n + m] = slab[:PAD].astype(jnp.bfloat16)
                edge_out[1, 2 * n + m] = slab[span - PAD :].astype(jnp.bfloat16)
            return carry

        lax.fori_loop(i * per, (i + 1) * per, turn, 0)

    to_left = copy(edge_out.at[0], edge_in.at[0], halo_send.at[0], halo_recv.at[0], (s - 1, d))
    to_right = copy(edge_out.at[1], edge_in.at[1], halo_send.at[1], halo_recv.at[1], (s + 1, d))

    @pl.when(has_left)
    def _():
        to_left.start()

    @pl.when(has_right)
    def _():
        to_right.start()

    for c in small:
        c.wait()
    stat[0] = jnp.zeros((span, LANES), jnp.float32)

    push(wbuf.at[d, piece_of(q), :], wbuf.at[d, piece_of(q), :], own_d2d.at[0, 0], own_d2d.at[1, 0], partner)
    push(wbuf.at[d, piece_of(q3), :], wbuf.at[d, piece_of(q3), :], own_d2d.at[0, 1], own_d2d.at[1, 1], partner)
    for n, p in ((2, q1), (3, q2)):
        own_loads[n].wait()
        push(wbuf.at[d, piece_of(p), :], wbuf.at[d, piece_of(p), :], own_d2d.at[0, n], own_d2d.at[1, n], partner)

    def halo():
        @pl.when(has_left)
        def _():
            to_right.wait_recv()
            gpad[:, 0:PAD, :] = edge_in[1].astype(jnp.float32)

        @pl.when(jnp.logical_not(has_left))
        def _():
            gpad[:, 0:PAD, :] = jnp.zeros((slabs, PAD, LANES), jnp.float32)

        @pl.when(has_right)
        def _():
            to_left.wait_recv()
            gpad[:, PAD + span :, :] = edge_in[0].astype(jnp.float32)

        @pl.when(jnp.logical_not(has_right))
        def _():
            gpad[:, PAD + span :, :] = jnp.zeros((slabs, PAD, LANES), jnp.float32)

    tile = min(LANES, span)

    def conv_slab(n, carry):
        lanes = pl.ds(pl.multiple_of(n * LANES, LANES), LANES)

        def tokens(t, inner):
            base = t * tile
            running = jnp.zeros((tile, LANES), jnp.float32)
            for j in range(taps_n):
                weight = taps[pl.ds(j, 1), lanes]
                running = running + weight * gpad[n, pl.ds(base + (PAD - half + j), tile), :]
            rounded = running.astype(jnp.bfloat16).astype(jnp.float32)
            at_token = pl.ds(pl.multiple_of(base, tile), tile)
            mixed[n, at_token, :] = rounded
            stat[0, at_token, :] += rounded
            return inner

        return lax.fori_loop(0, span // tile, tokens, carry)

    parts = 8

    def conv(i):
        return lambda: lax.fori_loop(i * slabs // parts, (i + 1) * slabs // parts, conv_slab, 0)

    def norm():
        mean = jnp.sum(stat[0], axis=1, keepdims=True) * (1.0 / channels)
        stat[0] = jnp.broadcast_to(mean, (span, LANES))
        stat[1] = jnp.zeros((span, LANES), jnp.float32)

        def spread(n, carry):
            apart = mixed[n] - stat[0]
            stat[1] += apart * apart
            return carry

        lax.fori_loop(0, slabs, spread, 0)
        variance = jnp.sum(stat[1], axis=1, keepdims=True) * (1.0 / channels)
        stat[1] = jnp.broadcast_to(lax.rsqrt(variance + 1e-05), (span, LANES))

    def activate():
        def one(n, carry):
            lanes = pl.ds(pl.multiple_of(n * LANES, LANES), LANES)
            normed = (mixed[n] - stat[0]) * stat[1]
            normed = normed * gain[:, lanes] + shift[:, lanes]
            act[:, lanes] = (normed * jax.nn.sigmoid(normed)).astype(jnp.bfloat16)
            return carry

        lax.fori_loop(0, slabs, one, 0)

    cols = min(width, 2 * LANES)

    def sweep(block, body):
        def columns(n, carry):
            at_col = pl.ds(pl.multiple_of(n * cols, cols), cols)
            at_out = pl.ds(pl.multiple_of(block * width + n * cols, cols), cols)
            body(at_col, at_out)
            return carry

        lax.fori_loop(0, width // cols, columns, 0)

    def product(block):
        def body(at_col, at_out):
            out[:, at_out] = jnp.dot(
                act[...], wbuf[block, :, at_col], preferred_element_type=jnp.float32
            ).astype(out.dtype)

        sweep(block, body)

    def slice_dot(block, p, at_col):
        return jnp.dot(
            act[:, piece_of(p)], wbuf[block, piece_of(p), at_col],
            preferred_element_type=jnp.float32,
        )

    def early(slot, block):
        def body(at_col, at_out):
            total = slice_dot(block, q, at_col) + slice_dot(block, q1, at_col)
            part[slot, :, at_col] = total + slice_dot(block, q2, at_col)

        sweep(block, body)

    def late(slot, block):
        def body(at_col, at_out):
            total = part[slot, :, at_col] + slice_dot(block, q3, at_col)
            out[:, at_out] = total.astype(out.dtype)

        sweep(block, body)

    def near(k):
        return ((g + groups - k) % groups) * 2 + core

    def far(k):
        return ((g + groups - k) % groups) * 2 + 1 - core

    def from_partner(k, n, p):
        for i in range(CHUNKS):
            m = n * CHUNKS + i
            landed(far(k), p, i, d_send.at[k - 1, m], d_recv.at[k - 1, m])

    def product_other():
        for n, p in enumerate((q, q3, q1, q2)):
            ref = wbuf.at[other, piece_of(p), :]
            copy(ref, ref, own_d2d.at[0, n], own_d2d.at[1, n], partner).wait_recv()
        product(other)

    def early_far(k):
        for n, p in enumerate((q, q1, q2)):
            from_partner(k, n, p)
        early(2 * k - 1, far(k))

    plan.append((3.6, halo))
    for i in range(parts):
        plan.append((4.6 + 0.75 * i, conv(i)))
    plan.append((10.7, norm))
    plan.append((11.2, activate))
    plan.append((11.7, lambda: product(d)))
    plan.append((12.2, product_other))
    for k in range(1, groups):
        plan.append((12.8, lambda k=k: early(2 * k - 2, near(k))))
        plan.append((13.1, lambda k=k: early_far(k)))
    for _, action in sorted(plan, key=lambda entry: entry[0]):
        action()
    for k in range(1, groups):
        late(2 * k - 2, near(k))
        from_partner(k, 3, q3)
        late(2 * k - 1, far(k))

    for c in sends:
        c.wait_send()

    @pl.when(has_left)
    def _():
        to_left.wait_send()

    @pl.when(has_right)
    def _():
        to_right.wait_send()


def solution(mesh):
    n_sp, n_dp = mesh.shape["sp"], mesh.shape["dp"]

    def per_device(lin_pre, gate_pre, w_depth, ln_gain, ln_shift, w_out):
        channels, span = lin_pre.shape
        width = w_out.shape[1]
        far = n_dp // 2 - 1
        slabs = channels // LANES
        dma = pltpu.SemaphoreType.DMA
        vmem = pl.BlockSpec(memory_space=pltpu.VMEM)
        hbm = pl.BlockSpec(memory_space=pl.ANY)
        return pl.pallas_call(
            functools.partial(kernel, n_sp, n_dp),
            out_shape=pltpu.VMEM((span, n_dp * width), jnp.bfloat16),
            in_specs=[hbm] * 6,
            out_specs=vmem,
            scratch_shapes=[
                pltpu.VMEM((channels, span), jnp.bfloat16),
                pltpu.VMEM((channels, span), jnp.bfloat16),
                pltpu.VMEM(w_depth.shape, jnp.float32),
                pltpu.VMEM((1, channels), jnp.float32),
                pltpu.VMEM((1, channels), jnp.float32),
                pltpu.VMEM((slabs, span + 2 * PAD, LANES), jnp.float32),
                pltpu.VMEM((slabs, span, LANES), jnp.float32),
                pltpu.VMEM((span, channels), jnp.bfloat16),
                pltpu.VMEM((n_dp, channels, width), jnp.bfloat16),
                pltpu.VMEM((2, span, LANES), jnp.float32),
                pltpu.VMEM((2 * far, span, width), jnp.float32),
                pltpu.VMEM((2, slabs, PAD, LANES), jnp.bfloat16),
                pltpu.VMEM((2, slabs, PAD, LANES), jnp.bfloat16),
                dma((2, 4)),
                dma((3,)),
                dma((4,)),
                dma((2, 4)),
                dma((2,)),
                dma((2,)),
                dma((far, CHUNKS + BY_Y)),
                dma((far, CHUNKS + BY_Y)),
                dma((far, CHUNKS + BY_X)),
                dma((far, CHUNKS + BY_X)),
                dma((far, CHUNKS + BY_Z)),
                dma((far, CHUNKS + BY_Z)),
                dma((far, 4 * CHUNKS)),
                dma((far, 4 * CHUNKS)),
            ],
            compiler_params=pltpu.CompilerParams(
                collective_id=0, has_side_effects=True, vmem_limit_bytes=60 * 2**20
            ),
            name="conv_module",
        )(lin_pre, gate_pre, w_depth, ln_gain[None, :], ln_shift[None, :], w_out)

    in_specs = (P(None, ("dp", "sp")), P(None, ("dp", "sp")), P(), P(), P(), P(None, "dp"))
    out_specs = P(("dp", "sp"), None)
    return jax.shard_map(
        per_device, mesh=mesh, in_specs=in_specs, out_specs=out_specs, check_vma=False
    )
```

```python
import functools

import jax
import jax.numpy as jnp
from jax import lax
from jax.experimental import pallas as pl
from jax.experimental.pallas import tpu as pltpu
from jax.sharding import PartitionSpec as P

MESH = pl.DeviceIdType.MESH
LANES = 128
PAD = 16
CHUNKS = 16
BY_X = 3
BY_Z = 4
BY_Y = CHUNKS - BY_X - BY_Z


def kernel(
    n_sp, n_dp, lin_hbm, gate_hbm, taps_hbm, gain_hbm, shift_hbm, w_hbm, out,
    lin_v, gate_v, taps, gain, shift, gpad, mixed, act, wbuf, stat, part, edge_out, edge_in,
    in_sem, small_sem, own_sem, own_d2d, halo_send, halo_recv,
    y_send, y_recv, x_send, x_recv, z_send, z_recv, d_send, d_recv,
):
    channels, span = lin_hbm.shape
    taps_n = taps.shape[0]
    half = (taps_n - 1) // 2
    width = w_hbm.shape[1]
    slabs = channels // LANES
    s = lax.axis_index("sp")
    d = lax.axis_index("dp")
    g, core = d // 2, d % 2
    groups = n_dp // 2
    partner = (s, g * 2 + 1 - core)
    other = g * 2 + 1 - core
    hi = (s // 2) % 2
    flip1 = s + 1 - 2 * (s % 2)
    flip2 = s + 2 - 4 * hi
    q = s % 4
    q1 = q + 1 - 2 * (s % 2)
    q2 = q + 2 - 4 * hi
    q3 = 3 - q
    piece = channels // 4
    rows = piece // CHUNKS

    barrier = pltpu.get_barrier_semaphore()
    peers = [partner, (flip1, d), (flip2, d)]
    for k in range(1, groups):
        peers.append((s, ((g + k) % groups) * 2 + core))
    for peer in peers:
        pl.semaphore_signal(barrier, inc=1, device_id=peer, device_id_type=MESH)
    has_left, has_right = s > 0, s < n_sp - 1

    @pl.when(has_left)
    def _():
        pl.semaphore_signal(barrier, inc=1, device_id=(s - 1, d), device_id_type=MESH)

    @pl.when(has_right)
    def _():
        pl.semaphore_signal(barrier, inc=1, device_id=(s + 1, d), device_id_type=MESH)

    n_peers = len(peers) + jnp.where(has_left, 1, 0) + jnp.where(has_right, 1, 0)

    def load(src, dst, sem):
        c = pltpu.make_async_copy(src, dst, sem)
        c.start()
        return c

    def piece_of(p):
        return pl.ds(pl.multiple_of(p * piece, piece), piece)

    def own_piece(n, p):
        return load(w_hbm.at[piece_of(p), :], wbuf.at[d, piece_of(p), :], own_sem.at[n])

    own_loads = [own_piece(0, q)]
    in_rows = channels // 4
    loads = []
    for i in range(4):
        cut = pl.ds(i * in_rows, in_rows)
        loads.append(load(gate_hbm.at[cut, :], gate_v.at[cut, :], in_sem.at[0, i]))
        loads.append(load(lin_hbm.at[cut, :], lin_v.at[cut, :], in_sem.at[1, i]))
    own_loads.append(own_piece(1, q3))
    small = [
        load(src, dst, small_sem.at[n])
        for n, (src, dst) in enumerate(((taps_hbm, taps), (gain_hbm, gain), (shift_hbm, shift)))
    ]
    own_loads.append(own_piece(2, q1))
    own_loads.append(own_piece(3, q2))

    def at(block, p, i):
        start = pl.multiple_of(p * piece + i * rows, rows)
        return wbuf.at[block, pl.ds(start, rows), :]

    def copy(src, dst, send, recv, device):
        return pltpu.make_async_remote_copy(
            src_ref=src, dst_ref=dst, send_sem=send, recv_sem=recv,
            device_id=device, device_id_type=MESH,
        )

    def push(*args):
        copy(*args).start()

    own_loads[0].wait()
    pl.semaphore_wait(barrier, n_peers)

    b_part = list(range(0, BY_X))
    c_part = list(range(BY_X, BY_X + BY_Z))
    a_part = list(range(BY_X + BY_Z, CHUNKS))

    def send_y(p, i, m):
        for k in range(1, groups):
            target = (s, ((g + k) % groups) * 2 + core)
            push(at(d, p, i), at(d, p, i), y_send.at[k - 1], y_recv.at[k - 1, m], target)

    for i in range(CHUNKS):
        send_y(q, i, i)
    own_loads[1].wait()
    for n, i in enumerate(a_part):
        send_y(q3, i, CHUNKS + n)

    def landed(block, p, i, send, recv):
        ref = at(block, p, i)
        copy(ref, ref, send, recv, partner).wait_recv()
        return ref

    def to_partner(ref, k, n):
        push(ref, ref, d_send.at[k - 1], d_recv.at[k - 1, n], partner)

    def event(kind, k, i):
        def run():
            block = ((g + groups - k) % groups) * 2 + core
            if kind == "y":
                ref = landed(block, q, i, y_send.at[k - 1], y_recv.at[k - 1, i])
                push(ref, ref, x_send.at[k - 1], x_recv.at[k - 1, i], (flip1, d))
                push(ref, ref, z_send.at[k - 1], z_recv.at[k - 1, i], (flip2, d))
                to_partner(ref, k, 0)
            elif kind == "x":
                ref = landed(block, q1, i, x_send.at[k - 1], x_recv.at[k - 1, i])
                if i in c_part:
                    m = CHUNKS + i - BY_X
                    push(ref, ref, z_send.at[k - 1], z_recv.at[k - 1, m], (flip2, d))
                to_partner(ref, k, 0)
            elif kind == "z":
                ref = landed(block, q2, i, z_send.at[k - 1], z_recv.at[k - 1, i])
                if i in b_part:
                    m = CHUNKS + i
                    push(ref, ref, x_send.at[k - 1], x_recv.at[k - 1, m], (flip1, d))
                to_partner(ref, k, 0)
            elif kind == "yd":
                m = CHUNKS + i - BY_X - BY_Z
                ref = landed(block, q3, i, y_send.at[k - 1], y_recv.at[k - 1, m])
                to_partner(ref, k, 1)
            elif kind == "xd":
                m = CHUNKS + i
                ref = landed(block, q3, i, x_send.at[k - 1], x_recv.at[k - 1, m])
                to_partner(ref, k, 1)
            else:
                m = CHUNKS + i - BY_X
                ref = landed(block, q3, i, z_send.at[k - 1], z_recv.at[k - 1, m])
                to_partner(ref, k, 1)

        return run

    plan = []
    unit = 11.2 / CHUNKS
    first_y, first_z, first_x = 1.9 + unit, 3.9 + 2 * unit, 4.4 + 2 * unit
    for k in range(1, groups):
        for i in range(CHUNKS):
            plan.append((first_y + unit * i, event("y", k, i)))
            later = 1.6 if unit * i < 8.4 else 0.6
            plan.append((first_z + unit * i + later, event("z", k, i)))
            plan.append((first_x + unit * i + later, event("x", k, i)))
        for n, i in enumerate(a_part):
            plan.append((first_y + unit * (CHUNKS + n), event("yd", k, i)))
        for n, i in enumerate(c_part):
            plan.append((first_z + unit * (CHUNKS + n), event("zd", k, i)))
        for n, i in enumerate(b_part):
            plan.append((first_x + unit * (CHUNKS + n), event("xd", k, i)))

    step = 2 * LANES
    eye = (
        lax.broadcasted_iota(jnp.int32, (span, span), 0)
        == lax.broadcasted_iota(jnp.int32, (span, span), 1)
    ).astype(jnp.float32).astype(jnp.bfloat16)

    for i in range(4):
        loads[2 * i].wait()
        loads[2 * i + 1].wait()
        per = in_rows // step

        def turn(n, carry):
            at_row = pl.multiple_of(n * step, step)
            cut = pl.ds(at_row, step)
            glu = (
                lin_v[cut, :].astype(jnp.float32)
                * jax.nn.sigmoid(gate_v[cut, :].astype(jnp.float32))
            ).astype(jnp.bfloat16)
            turned = lax.dot_general(
                eye, glu, (((1,), (1,)), ((), ())), preferred_element_type=jnp.float32
            )
            for m in range(2):
                slab = turned[:, m * LANES : (m + 1) * LANES]
                gpad[2 * n + m, pl.ds(PAD, span), :] = slab
                edge_out[0, 2 * n + m] = slab[:PAD].astype(jnp.bfloat16)
                edge_out[1, 2 * n + m] = slab[span - PAD :].astype(jnp.bfloat16)
            return carry

        lax.fori_loop(i * per, (i + 1) * per, turn, 0)

    to_left = copy(edge_out.at[0], edge_in.at[0], halo_send.at[0], halo_recv.at[0], (s - 1, d))
    to_right = copy(edge_out.at[1], edge_in.at[1], halo_send.at[1], halo_recv.at[1], (s + 1, d))

    @pl.when(has_left)
    def _():
        to_left.start()

    @pl.when(has_right)
    def _():
        to_right.start()

    for c in small:
        c.wait()
    stat[0] = jnp.zeros((span, LANES), jnp.float32)

    own_loads[2].wait()
    own_loads[3].wait()
    push(wbuf.at[d], wbuf.at[d], own_d2d.at[0], own_d2d.at[1], partner)

    def halo():
        @pl.when(has_left)
        def _():
            to_right.wait_recv()
            gpad[:, 0:PAD, :] = edge_in[1].astype(jnp.float32)

        @pl.when(jnp.logical_not(has_left))
        def _():
            gpad[:, 0:PAD, :] = jnp.zeros((slabs, PAD, LANES), jnp.float32)

        @pl.when(has_right)
        def _():
            to_left.wait_recv()
            gpad[:, PAD + span :, :] = edge_in[0].astype(jnp.float32)

        @pl.when(jnp.logical_not(has_right))
        def _():
            gpad[:, PAD + span :, :] = jnp.zeros((slabs, PAD, LANES), jnp.float32)

    def taps_sum(n, base, count):
        lanes = pl.ds(pl.multiple_of(n * LANES, LANES), LANES)
        running = jnp.zeros((count, LANES), jnp.float32)
        for j in range(taps_n):
            weight = taps[pl.ds(j, 1), lanes]
            running = running + weight * gpad[n, pl.ds(base + (PAD - half + j), count), :]
        rounded = running.astype(jnp.bfloat16).astype(jnp.float32)
        at_token = pl.ds(pl.multiple_of(base, PAD), count)
        mixed[n, at_token, :] = rounded
        stat[0, at_token, :] += rounded

    inner = span - 2 * PAD
    tiles = next(m for m in range(2, inner) if inner % m == 0 and inner // m <= LANES and inner // m % PAD == 0)
    tile = inner // tiles

    def conv_slab(n, carry):
        def tokens(m, within):
            taps_sum(n, PAD + m * tile, tile)
            return within

        return lax.fori_loop(0, tiles, tokens, carry)

    def edges():
        def one(n, carry):
            def side(m, within):
                taps_sum(n, m * (span - PAD), PAD)
                return within

            return lax.fori_loop(0, 2, side, carry, unroll=True)

        lax.fori_loop(0, slabs, one, 0)

    parts = 8

    def conv(i):
        return lambda: lax.fori_loop(i * slabs // parts, (i + 1) * slabs // parts, conv_slab, 0)

    def norm():
        mean = jnp.sum(stat[0], axis=1, keepdims=True) * (1.0 / channels)
        stat[0] = jnp.broadcast_to(mean, (span, LANES))
        stat[1] = jnp.zeros((span, LANES), jnp.float32)

        def spread(n, carry):
            apart = mixed[n] - stat[0]
            stat[1] += apart * apart
            return carry

        lax.fori_loop(0, slabs, spread, 0)
        variance = jnp.sum(stat[1], axis=1, keepdims=True) * (1.0 / channels)
        stat[1] = jnp.broadcast_to(lax.rsqrt(variance + 1e-05), (span, LANES))

    def activate(h):
        def one(n, carry):
            lanes = pl.ds(pl.multiple_of(n * LANES, LANES), LANES)
            normed = (mixed[n] - stat[0]) * stat[1]
            normed = normed * gain[:, lanes] + shift[:, lanes]
            act[:, lanes] = (normed * jax.nn.sigmoid(normed)).astype(jnp.bfloat16)
            return carry

        lax.fori_loop(h * slabs // 2, (h + 1) * slabs // 2, one, 0)

    cols = min(width, 2 * LANES)

    halves = width // cols

    def sweep(block, body, first=0, count=halves):
        def columns(n, carry):
            at_col = pl.ds(pl.multiple_of(n * cols, cols), cols)
            at_out = pl.ds(pl.multiple_of(block * width + n * cols, cols), cols)
            body(at_col, at_out)
            return carry

        lax.fori_loop(first, first + count, columns, 0)

    def product(block, n):
        def body(at_col, at_out):
            out[:, at_out] = jnp.dot(
                act[...], wbuf[block, :, at_col], preferred_element_type=jnp.float32
            ).astype(out.dtype)

        sweep(block, body, n, 1)

    def slice_dot(block, p, at_col):
        return jnp.dot(
            act[:, piece_of(p)], wbuf[block, piece_of(p), at_col],
            preferred_element_type=jnp.float32,
        )

    def early(slot, block):
        def body(at_col, at_out):
            total = slice_dot(block, q, at_col) + slice_dot(block, q1, at_col)
            part[slot, :, at_col] = total + slice_dot(block, q2, at_col)

        sweep(block, body)

    def late(slot, block):
        def body(at_col, at_out):
            total = part[slot, :, at_col] + slice_dot(block, q3, at_col)
            out[:, at_out] = total.astype(out.dtype)

        sweep(block, body)

    def near(k):
        return ((g + groups - k) % groups) * 2 + core

    def far(k):
        return ((g + groups - k) % groups) * 2 + 1 - core

    def from_partner(k, n, size):
        ref = wbuf.at[far(k), pl.ds(0, size * piece), :]
        copy(ref, ref, d_send.at[k - 1], d_recv.at[k - 1, n], partner).wait_recv()

    def early_far(k):
        from_partner(k, 0, 3)
        early(2 * k - 1, far(k))

    def take_other():
        copy(wbuf.at[other], wbuf.at[other], own_d2d.at[0], own_d2d.at[1], partner).wait_recv()

    for i in range(parts):
        plan.append((1.5 + 0.6 * i, conv(i)))
    plan.append((6.3, halo))
    plan.append((6.4, edges))
    plan.append((7.3, norm))
    plan.append((7.9, lambda: activate(0)))
    plan.append((8.3, lambda: activate(1)))
    for n in range(halves):
        plan.append((8.7 + 1.0 * n / halves, lambda n=n: product(d, n)))
        plan.append((9.8 + 1.0 * n / halves, lambda n=n: product(other, n)))
    plan.append((9.75, take_other))
    for k in range(1, groups):
        plan.append((first_x + unit * CHUNKS, lambda k=k: early(2 * k - 2, near(k))))
        plan.append((first_x + unit * (CHUNKS + 1), lambda k=k: early_far(k)))
    for _, action in sorted(plan, key=lambda entry: entry[0]):
        action()
    for k in range(1, groups):
        late(2 * k - 2, near(k))
        from_partner(k, 1, 1)
        late(2 * k - 1, far(k))

    def sent(sem, size):
        ref = wbuf.at[d, pl.ds(0, size * rows), :]
        copy(ref, ref, sem, own_d2d.at[1], partner).wait_send()

    for k in range(1, groups):
        sent(y_send.at[k - 1], CHUNKS + BY_Y)
        sent(x_send.at[k - 1], CHUNKS + BY_X)
        sent(z_send.at[k - 1], CHUNKS + BY_Z)
        sent(d_send.at[k - 1], 4 * CHUNKS)
    sent(own_d2d.at[0], 4 * CHUNKS)

    @pl.when(has_left)
    def _():
        to_left.wait_send()

    @pl.when(has_right)
    def _():
        to_right.wait_send()


def solution(mesh):
    n_sp, n_dp = mesh.shape["sp"], mesh.shape["dp"]

    def per_device(lin_pre, gate_pre, w_depth, ln_gain, ln_shift, w_out):
        channels, span = lin_pre.shape
        width = w_out.shape[1]
        far = n_dp // 2 - 1
        slabs = channels // LANES
        dma = pltpu.SemaphoreType.DMA
        vmem = pl.BlockSpec(memory_space=pltpu.VMEM)
        hbm = pl.BlockSpec(memory_space=pl.ANY)
        return pl.pallas_call(
            functools.partial(kernel, n_sp, n_dp),
            out_shape=pltpu.VMEM((span, n_dp * width), jnp.bfloat16),
            in_specs=[hbm] * 6,
            out_specs=vmem,
            scratch_shapes=[
                pltpu.VMEM((channels, span), jnp.bfloat16),
                pltpu.VMEM((channels, span), jnp.bfloat16),
                pltpu.VMEM(w_depth.shape, jnp.float32),
                pltpu.VMEM((1, channels), jnp.float32),
                pltpu.VMEM((1, channels), jnp.float32),
                pltpu.VMEM((slabs, span + 2 * PAD, LANES), jnp.float32),
                pltpu.VMEM((slabs, span, LANES), jnp.float32),
                pltpu.VMEM((span, channels), jnp.bfloat16),
                pltpu.VMEM((n_dp, channels, width), jnp.bfloat16),
                pltpu.VMEM((2, span, LANES), jnp.float32),
                pltpu.VMEM((2 * far, span, width), jnp.float32),
                pltpu.VMEM((2, slabs, PAD, LANES), jnp.bfloat16),
                pltpu.VMEM((2, slabs, PAD, LANES), jnp.bfloat16),
                dma((2, 4)),
                dma((3,)),
                dma((4,)),
                dma((2,)),
                dma((2,)),
                dma((2,)),
                dma((far,)),
                dma((far, CHUNKS + BY_Y)),
                dma((far,)),
                dma((far, CHUNKS + BY_X)),
                dma((far,)),
                dma((far, CHUNKS + BY_Z)),
                dma((far,)),
                dma((far, 2)),
            ],
            compiler_params=pltpu.CompilerParams(
                collective_id=0, has_side_effects=True, vmem_limit_bytes=60 * 2**20
            ),
            name="conv_module",
        )(lin_pre, gate_pre, w_depth, ln_gain[None, :], ln_shift[None, :], w_out)

    in_specs = (P(None, ("dp", "sp")), P(None, ("dp", "sp")), P(), P(), P(), P(None, "dp"))
    out_specs = P(("dp", "sp"), None)
    return jax.shard_map(
        per_device, mesh=mesh, in_specs=in_specs, out_specs=out_specs, check_vma=False
    )
```

```python
import functools

import jax
import jax.numpy as jnp
from jax import lax
from jax.experimental import pallas as pl
from jax.experimental.pallas import tpu as pltpu
from jax.sharding import PartitionSpec as P

MESH = pl.DeviceIdType.MESH
LANES = 128
PAD = 16
CHUNKS = 16
BY_X = 2
BY_Z = 3
BY_Y = CHUNKS - BY_X - BY_Z
SOON = 3 * CHUNKS // 4


def kernel(
    n_sp, n_dp, lin_hbm, gate_hbm, taps_hbm, gain_hbm, shift_hbm, w_hbm, out,
    lin_v, gate_v, taps, gain, shift, gpad, mixed, act, wbuf, stat, part, edge_out, edge_in,
    in_sem, small_sem, own_sem, own_d2d, halo_send, halo_recv,
    y_send, y_recv, x_send, x_recv, z_send, z_recv, d_send, d_recv,
):
    channels, span = lin_hbm.shape
    taps_n = taps.shape[0]
    half = (taps_n - 1) // 2
    width = w_hbm.shape[1]
    slabs = channels // LANES
    s = lax.axis_index("sp")
    d = lax.axis_index("dp")
    g, core = d // 2, d % 2
    groups = n_dp // 2
    partner = (s, g * 2 + 1 - core)
    other = g * 2 + 1 - core
    hi = (s // 2) % 2
    flip1 = s + 1 - 2 * (s % 2)
    flip2 = s + 2 - 4 * hi
    q = s % 4
    q1 = q + 1 - 2 * (s % 2)
    q2 = q + 2 - 4 * hi
    q3 = 3 - q
    piece = channels // 4
    rows = piece // CHUNKS

    barrier = pltpu.get_barrier_semaphore()
    peers = [partner, (flip1, d), (flip2, d)]
    for k in range(1, groups):
        peers.append((s, ((g + k) % groups) * 2 + core))
    for peer in peers:
        pl.semaphore_signal(barrier, inc=1, device_id=peer, device_id_type=MESH)
    has_left, has_right = s > 0, s < n_sp - 1

    @pl.when(has_left)
    def _():
        pl.semaphore_signal(barrier, inc=1, device_id=(s - 1, d), device_id_type=MESH)

    @pl.when(has_right)
    def _():
        pl.semaphore_signal(barrier, inc=1, device_id=(s + 1, d), device_id_type=MESH)

    n_peers = len(peers) + jnp.where(has_left, 1, 0) + jnp.where(has_right, 1, 0)

    def load(src, dst, sem):
        c = pltpu.make_async_copy(src, dst, sem)
        c.start()
        return c

    def piece_of(p):
        return pl.ds(pl.multiple_of(p * piece, piece), piece)

    def own_piece(n, p):
        return load(w_hbm.at[piece_of(p), :], wbuf.at[d, piece_of(p), :], own_sem.at[n])

    own_loads = [own_piece(0, q)]
    in_rows = channels // 4
    loads = []
    for i in range(4):
        cut = pl.ds(i * in_rows, in_rows)
        loads.append(load(gate_hbm.at[cut, :], gate_v.at[cut, :], in_sem.at[0, i]))
        loads.append(load(lin_hbm.at[cut, :], lin_v.at[cut, :], in_sem.at[1, i]))
    own_loads.append(own_piece(1, q3))
    small = [
        load(src, dst, small_sem.at[n])
        for n, (src, dst) in enumerate(((taps_hbm, taps), (gain_hbm, gain), (shift_hbm, shift)))
    ]
    own_loads.append(own_piece(2, q1))
    own_loads.append(own_piece(3, q2))

    def at(block, p, i):
        start = pl.multiple_of(p * piece + i * rows, rows)
        return wbuf.at[block, pl.ds(start, rows), :]

    def copy(src, dst, send, recv, device):
        return pltpu.make_async_remote_copy(
            src_ref=src, dst_ref=dst, send_sem=send, recv_sem=recv,
            device_id=device, device_id_type=MESH,
        )

    def push(*args):
        copy(*args).start()

    own_loads[0].wait()
    pl.semaphore_wait(barrier, n_peers)

    b_part = list(range(0, BY_X))
    c_part = list(range(BY_X, BY_X + BY_Z))
    a_part = list(range(BY_X + BY_Z, CHUNKS))

    def send_y(p, i, m):
        for k in range(1, groups):
            target = (s, ((g + k) % groups) * 2 + core)
            push(at(d, p, i), at(d, p, i), y_send.at[k - 1], y_recv.at[k - 1, m], target)

    for i in range(CHUNKS):
        send_y(q, i, i)
    own_loads[1].wait()
    for n, i in enumerate(a_part):
        send_y(q3, i, CHUNKS + n)

    def landed(block, p, i, send, recv):
        ref = at(block, p, i)
        copy(ref, ref, send, recv, partner).wait_recv()
        return ref

    def to_partner(ref, k, n):
        push(ref, ref, d_send.at[k - 1], d_recv.at[k - 1, n], partner)

    def event(kind, k, i):
        def run():
            block = ((g + groups - k) % groups) * 2 + core
            if kind == "y":
                ref = landed(block, q, i, y_send.at[k - 1], y_recv.at[k - 1, i])
                push(ref, ref, x_send.at[k - 1], x_recv.at[k - 1, i], (flip1, d))
                push(ref, ref, z_send.at[k - 1], z_recv.at[k - 1, i], (flip2, d))
                to_partner(ref, k, 0)
            elif kind == "x":
                ref = landed(block, q1, i, x_send.at[k - 1], x_recv.at[k - 1, i])
                if i in c_part:
                    m = CHUNKS + i - BY_X
                    push(ref, ref, z_send.at[k - 1], z_recv.at[k - 1, m], (flip2, d))
                to_partner(ref, k, 1 if i < SOON else 2)
            elif kind == "z":
                ref = landed(block, q2, i, z_send.at[k - 1], z_recv.at[k - 1, i])
                if i in b_part:
                    m = CHUNKS + i
                    push(ref, ref, x_send.at[k - 1], x_recv.at[k - 1, m], (flip1, d))
                to_partner(ref, k, 1 if i < SOON else 2)
            elif kind == "yd":
                m = CHUNKS + i - BY_X - BY_Z
                ref = landed(block, q3, i, y_send.at[k - 1], y_recv.at[k - 1, m])
                to_partner(ref, k, 2)
            elif kind == "xd":
                m = CHUNKS + i
                ref = landed(block, q3, i, x_send.at[k - 1], x_recv.at[k - 1, m])
                to_partner(ref, k, 2)
            else:
                m = CHUNKS + i - BY_X
                ref = landed(block, q3, i, z_send.at[k - 1], z_recv.at[k - 1, m])
                to_partner(ref, k, 2)

        return run

    plan = []
    unit = 11.2 / CHUNKS
    first_y, first_z, first_x = 1.9 + unit, 3.9 + 2 * unit, 4.4 + 2 * unit
    for k in range(1, groups):
        for i in range(CHUNKS):
            plan.append((first_y + unit * i, event("y", k, i)))
            later = 1.0
            plan.append((first_z + unit * i + later, event("z", k, i)))
            plan.append((first_x + unit * i + later, event("x", k, i)))
        for n, i in enumerate(a_part):
            plan.append((first_y + unit * (CHUNKS + n), event("yd", k, i)))
        for n, i in enumerate(c_part):
            plan.append((first_z + unit * (CHUNKS + n), event("zd", k, i)))
        for n, i in enumerate(b_part):
            plan.append((first_x + unit * (CHUNKS + n), event("xd", k, i)))

    step = 2 * LANES
    eye = (
        lax.broadcasted_iota(jnp.int32, (span, span), 0)
        == lax.broadcasted_iota(jnp.int32, (span, span), 1)
    ).astype(jnp.float32).astype(jnp.bfloat16)

    for i in range(4):
        loads[2 * i].wait()
        loads[2 * i + 1].wait()
        per = in_rows // step

        def turn(n, carry):
            at_row = pl.multiple_of(n * step, step)
            cut = pl.ds(at_row, step)
            glu = (
                lin_v[cut, :].astype(jnp.float32)
                * jax.nn.sigmoid(gate_v[cut, :].astype(jnp.float32))
            ).astype(jnp.bfloat16)
            turned = lax.dot_general(
                eye, glu, (((1,), (1,)), ((), ())), preferred_element_type=jnp.float32
            )
            for m in range(2):
                slab = turned[:, m * LANES : (m + 1) * LANES]
                gpad[2 * n + m, pl.ds(PAD, span), :] = slab
                edge_out[0, 2 * n + m] = slab[:PAD].astype(jnp.bfloat16)
                edge_out[1, 2 * n + m] = slab[span - PAD :].astype(jnp.bfloat16)
            return carry

        lax.fori_loop(i * per, (i + 1) * per, turn, 0)

    to_left = copy(edge_out.at[0], edge_in.at[0], halo_send.at[0], halo_recv.at[0], (s - 1, d))
    to_right = copy(edge_out.at[1], edge_in.at[1], halo_send.at[1], halo_recv.at[1], (s + 1, d))

    @pl.when(has_left)
    def _():
        to_left.start()

    @pl.when(has_right)
    def _():
        to_right.start()

    for c in small:
        c.wait()
    stat[0] = jnp.zeros((span, LANES), jnp.float32)

    own_loads[2].wait()
    own_loads[3].wait()
    push(wbuf.at[d], wbuf.at[d], own_d2d.at[0], own_d2d.at[1], partner)

    def halo():
        @pl.when(has_left)
        def _():
            to_right.wait_recv()
            gpad[:, 0:PAD, :] = edge_in[1].astype(jnp.float32)

        @pl.when(jnp.logical_not(has_left))
        def _():
            gpad[:, 0:PAD, :] = jnp.zeros((slabs, PAD, LANES), jnp.float32)

        @pl.when(has_right)
        def _():
            to_left.wait_recv()
            gpad[:, PAD + span :, :] = edge_in[0].astype(jnp.float32)

        @pl.when(jnp.logical_not(has_right))
        def _():
            gpad[:, PAD + span :, :] = jnp.zeros((slabs, PAD, LANES), jnp.float32)

    def taps_sum(n, base, count):
        lanes = pl.ds(pl.multiple_of(n * LANES, LANES), LANES)
        running = jnp.zeros((count, LANES), jnp.float32)
        for j in range(taps_n):
            weight = taps[pl.ds(j, 1), lanes]
            running = running + weight * gpad[n, pl.ds(base + (PAD - half + j), count), :]
        rounded = running.astype(jnp.bfloat16).astype(jnp.float32)
        at_token = pl.ds(pl.multiple_of(base, PAD), count)
        mixed[n, at_token, :] = rounded
        stat[0, at_token, :] += rounded

    inner = span - 2 * PAD
    tiles = next(m for m in range(2, inner) if inner % m == 0 and inner // m <= LANES and inner // m % PAD == 0)
    tile = inner // tiles

    def conv_slab(n, carry):
        def tokens(m, within):
            taps_sum(n, PAD + m * tile, tile)
            return within

        return lax.fori_loop(0, tiles, tokens, carry)

    def edges():
        def one(n, carry):
            def side(m, within):
                taps_sum(n, m * (span - PAD), PAD)
                return within

            return lax.fori_loop(0, 2, side, carry, unroll=True)

        lax.fori_loop(0, slabs, one, 0)

    parts = 8

    def conv(i):
        return lambda: lax.fori_loop(i * slabs // parts, (i + 1) * slabs // parts, conv_slab, 0)

    def norm():
        mean = jnp.sum(stat[0], axis=1, keepdims=True) * (1.0 / channels)
        stat[0] = jnp.broadcast_to(mean, (span, LANES))
        stat[1] = jnp.zeros((span, LANES), jnp.float32)

        def spread(n, carry):
            apart = mixed[n] - stat[0]
            stat[1] += apart * apart
            return carry

        lax.fori_loop(0, slabs, spread, 0)
        variance = jnp.sum(stat[1], axis=1, keepdims=True) * (1.0 / channels)
        stat[1] = jnp.broadcast_to(lax.rsqrt(variance + 1e-05), (span, LANES))

    def activate(h):
        def one(n, carry):
            lanes = pl.ds(pl.multiple_of(n * LANES, LANES), LANES)
            normed = (mixed[n] - stat[0]) * stat[1]
            normed = normed * gain[:, lanes] + shift[:, lanes]
            act[:, lanes] = (normed * jax.nn.sigmoid(normed)).astype(jnp.bfloat16)
            return carry

        lax.fori_loop(h * slabs // 2, (h + 1) * slabs // 2, one, 0)

    cols = min(width, 2 * LANES)

    halves = width // cols

    def sweep(block, body, first=0, count=halves):
        def columns(n, carry):
            at_col = pl.ds(pl.multiple_of(n * cols, cols), cols)
            at_out = pl.ds(pl.multiple_of(block * width + n * cols, cols), cols)
            body(at_col, at_out)
            return carry

        lax.fori_loop(first, first + count, columns, 0)

    def product(block, n):
        def body(at_col, at_out):
            out[:, at_out] = jnp.dot(
                act[...], wbuf[block, :, at_col], preferred_element_type=jnp.float32
            ).astype(out.dtype)

        sweep(block, body, n, 1)

    def slice_dot(block, p, at_col, low=0, high=CHUNKS):
        at_row = pl.ds(pl.multiple_of(p * piece + low * rows, LANES), (high - low) * rows)
        return jnp.dot(
            act[:, at_row], wbuf[block, at_row, at_col], preferred_element_type=jnp.float32
        )

    def stage(which, slot, block):
        def body(at_col, at_out):
            if which == 0:
                part[slot, :, at_col] = slice_dot(block, q, at_col)
            elif which == 1:
                total = part[slot, :, at_col] + slice_dot(block, q1, at_col, 0, SOON)
                part[slot, :, at_col] = total + slice_dot(block, q2, at_col, 0, SOON)
            else:
                total = part[slot, :, at_col] + slice_dot(block, q1, at_col, SOON)
                total = total + slice_dot(block, q2, at_col, SOON)
                out[:, at_out] = (total + slice_dot(block, q3, at_col)).astype(out.dtype)

        sweep(block, body)

    def near(k):
        return ((g + groups - k) % groups) * 2 + core

    def far(k):
        return ((g + groups - k) % groups) * 2 + 1 - core

    late = CHUNKS - SOON
    shares = (CHUNKS, 2 * SOON, 2 * late + CHUNKS)

    def stage_near(which, k):
        stage(which, 2 * k - 2, near(k))

    def stage_far(which, k):
        ref = wbuf.at[far(k), pl.ds(0, shares[which] * rows), :]
        copy(ref, ref, d_send.at[k - 1], d_recv.at[k - 1, which], partner).wait_recv()
        stage(which, 2 * k - 1, far(k))

    def take_other():
        copy(wbuf.at[other], wbuf.at[other], own_d2d.at[0], own_d2d.at[1], partner).wait_recv()

    for i in range(parts):
        plan.append((1.5 + 0.6 * i, conv(i)))
    plan.append((6.3, halo))
    plan.append((6.4, edges))
    plan.append((7.3, norm))
    plan.append((7.9, lambda: activate(0)))
    plan.append((8.3, lambda: activate(1)))
    for n in range(halves):
        plan.append((8.7 + 1.0 * n / halves, lambda n=n: product(d, n)))
        plan.append((9.8 + 1.0 * n / halves, lambda n=n: product(other, n)))
    plan.append((9.75, take_other))
    for k in range(1, groups):
        for which, when in ((0, 13.2), (1, 14.6)):
            plan.append((when, lambda k=k, which=which: stage_near(which, k)))
            plan.append((when + 1.2, lambda k=k, which=which: stage_far(which, k)))
    for _, action in sorted(plan, key=lambda entry: entry[0]):
        action()
    for k in range(1, groups):
        stage_near(2, k)
        stage_far(2, k)

    def sent(sem, size):
        ref = wbuf.at[d, pl.ds(0, size * rows), :]
        copy(ref, ref, sem, own_d2d.at[1], partner).wait_send()

    for k in range(1, groups):
        sent(y_send.at[k - 1], CHUNKS + BY_Y)
        sent(x_send.at[k - 1], CHUNKS + BY_X)
        sent(z_send.at[k - 1], CHUNKS + BY_Z)
        sent(d_send.at[k - 1], 4 * CHUNKS)
    sent(own_d2d.at[0], 4 * CHUNKS)

    @pl.when(has_left)
    def _():
        to_left.wait_send()

    @pl.when(has_right)
    def _():
        to_right.wait_send()


def solution(mesh):
    n_sp, n_dp = mesh.shape["sp"], mesh.shape["dp"]

    def per_device(lin_pre, gate_pre, w_depth, ln_gain, ln_shift, w_out):
        channels, span = lin_pre.shape
        width = w_out.shape[1]
        far = n_dp // 2 - 1
        slabs = channels // LANES
        dma = pltpu.SemaphoreType.DMA
        vmem = pl.BlockSpec(memory_space=pltpu.VMEM)
        hbm = pl.BlockSpec(memory_space=pl.ANY)
        return pl.pallas_call(
            functools.partial(kernel, n_sp, n_dp),
            out_shape=pltpu.VMEM((span, n_dp * width), jnp.bfloat16),
            in_specs=[hbm] * 6,
            out_specs=vmem,
            scratch_shapes=[
                pltpu.VMEM((channels, span), jnp.bfloat16),
                pltpu.VMEM((channels, span), jnp.bfloat16),
                pltpu.VMEM(w_depth.shape, jnp.float32),
                pltpu.VMEM((1, channels), jnp.float32),
                pltpu.VMEM((1, channels), jnp.float32),
                pltpu.VMEM((slabs, span + 2 * PAD, LANES), jnp.float32),
                pltpu.VMEM((slabs, span, LANES), jnp.float32),
                pltpu.VMEM((span, channels), jnp.bfloat16),
                pltpu.VMEM((n_dp, channels, width), jnp.bfloat16),
                pltpu.VMEM((2, span, LANES), jnp.float32),
                pltpu.VMEM((2 * far, span, width), jnp.float32),
                pltpu.VMEM((2, slabs, PAD, LANES), jnp.bfloat16),
                pltpu.VMEM((2, slabs, PAD, LANES), jnp.bfloat16),
                dma((2, 4)),
                dma((3,)),
                dma((4,)),
                dma((2,)),
                dma((2,)),
                dma((2,)),
                dma((far,)),
                dma((far, CHUNKS + BY_Y)),
                dma((far,)),
                dma((far, CHUNKS + BY_X)),
                dma((far,)),
                dma((far, CHUNKS + BY_Z)),
                dma((far,)),
                dma((far, 3)),
            ],
            compiler_params=pltpu.CompilerParams(
                collective_id=0, has_side_effects=True, vmem_limit_bytes=60 * 2**20
            ),
            name="conv_module",
        )(lin_pre, gate_pre, w_depth, ln_gain[None, :], ln_shift[None, :], w_out)

    in_specs = (P(None, ("dp", "sp")), P(None, ("dp", "sp")), P(), P(), P(), P(None, "dp"))
    out_specs = P(("dp", "sp"), None)
    return jax.shard_map(
        per_device, mesh=mesh, in_specs=in_specs, out_specs=out_specs, check_vma=False
    )
```

```python
import functools

import jax
import jax.numpy as jnp
from jax import lax
from jax.experimental import pallas as pl
from jax.experimental.pallas import tpu as pltpu
from jax.sharding import PartitionSpec as P

MESH = pl.DeviceIdType.MESH
LANES = 128
PAD = 16
CHUNKS = 16
BY_X = 2
BY_Z = 3
BY_Y = CHUNKS - BY_X - BY_Z
SOON = 3 * CHUNKS // 4


def kernel(
    n_sp, n_dp, lin_hbm, gate_hbm, taps_hbm, gain_hbm, shift_hbm, w_hbm, out,
    lin_v, gate_v, taps, gain, shift, gpad, mixed, act, wbuf, stat, part, edge_out, edge_in,
    in_sem, small_sem, own_sem, own_d2d, halo_send, halo_recv,
    y_send, y_recv, x_send, x_recv, z_send, z_recv, d_send, d_recv,
):
    channels, span = lin_hbm.shape
    taps_n = taps.shape[0]
    half = (taps_n - 1) // 2
    width = w_hbm.shape[1]
    slabs = channels // LANES
    s = lax.axis_index("sp")
    d = lax.axis_index("dp")
    g, core = d // 2, d % 2
    groups = n_dp // 2
    partner = (s, g * 2 + 1 - core)
    other = g * 2 + 1 - core
    hi = (s // 2) % 2
    flip1 = s + 1 - 2 * (s % 2)
    flip2 = s + 2 - 4 * hi
    q = s % 4
    q1 = q + 1 - 2 * (s % 2)
    q2 = q + 2 - 4 * hi
    q3 = 3 - q
    piece = channels // 4
    rows = piece // CHUNKS

    barrier = pltpu.get_barrier_semaphore()
    peers = [partner, (flip1, d), (flip2, d)]
    for k in range(1, groups):
        peers.append((s, ((g + k) % groups) * 2 + core))
    for peer in peers:
        pl.semaphore_signal(barrier, inc=1, device_id=peer, device_id_type=MESH)
    has_left, has_right = s > 0, s < n_sp - 1

    @pl.when(has_left)
    def _():
        pl.semaphore_signal(barrier, inc=1, device_id=(s - 1, d), device_id_type=MESH)

    @pl.when(has_right)
    def _():
        pl.semaphore_signal(barrier, inc=1, device_id=(s + 1, d), device_id_type=MESH)

    n_peers = len(peers) + jnp.where(has_left, 1, 0) + jnp.where(has_right, 1, 0)

    def load(src, dst, sem):
        c = pltpu.make_async_copy(src, dst, sem)
        c.start()
        return c

    def piece_of(p):
        return pl.ds(pl.multiple_of(p * piece, piece), piece)

    def own_piece(n, p):
        return load(w_hbm.at[piece_of(p), :], wbuf.at[d, piece_of(p), :], own_sem.at[n])

    def own_cut(n, low, high):
        cut = pl.ds(pl.multiple_of(q * piece + low * rows, rows), (high - low) * rows)
        return load(w_hbm.at[cut, :], wbuf.at[d, cut, :], own_sem.at[n])

    head = CHUNKS // 8
    own_head = own_cut(4, 0, head)
    own_loads = [own_cut(0, head, CHUNKS)]
    in_rows = channels // 4
    loads = []
    for i in range(4):
        cut = pl.ds(i * in_rows, in_rows)
        loads.append(load(gate_hbm.at[cut, :], gate_v.at[cut, :], in_sem.at[0, i]))
        loads.append(load(lin_hbm.at[cut, :], lin_v.at[cut, :], in_sem.at[1, i]))
    own_loads.append(own_piece(1, q3))
    small = [
        load(src, dst, small_sem.at[n])
        for n, (src, dst) in enumerate(((taps_hbm, taps), (gain_hbm, gain), (shift_hbm, shift)))
    ]
    own_loads.append(own_piece(2, q1))
    own_loads.append(own_piece(3, q2))

    def at(block, p, i):
        start = pl.multiple_of(p * piece + i * rows, rows)
        return wbuf.at[block, pl.ds(start, rows), :]

    def copy(src, dst, send, recv, device):
        return pltpu.make_async_remote_copy(
            src_ref=src, dst_ref=dst, send_sem=send, recv_sem=recv,
            device_id=device, device_id_type=MESH,
        )

    def push(*args):
        copy(*args).start()

    own_head.wait()
    pl.semaphore_wait(barrier, n_peers)

    b_part = list(range(0, BY_X))
    c_part = list(range(BY_X, BY_X + BY_Z))
    a_part = list(range(BY_X + BY_Z, CHUNKS))

    def send_y(p, i, m):
        for k in range(1, groups):
            target = (s, ((g + k) % groups) * 2 + core)
            push(at(d, p, i), at(d, p, i), y_send.at[k - 1], y_recv.at[k - 1, m], target)

    for i in range(CHUNKS):
        if i == head:
            own_loads[0].wait()
        send_y(q, i, i)
    own_loads[1].wait()
    for n, i in enumerate(a_part):
        send_y(q3, i, CHUNKS + n)

    def landed(block, p, i, send, recv):
        ref = at(block, p, i)
        copy(ref, ref, send, recv, partner).wait_recv()
        return ref

    def to_partner(ref, k, n):
        push(ref, ref, d_send.at[k - 1], d_recv.at[k - 1, n], partner)

    def event(kind, k, i):
        def run():
            block = ((g + groups - k) % groups) * 2 + core
            if kind == "y":
                ref = landed(block, q, i, y_send.at[k - 1], y_recv.at[k - 1, i])
                push(ref, ref, x_send.at[k - 1], x_recv.at[k - 1, i], (flip1, d))
                push(ref, ref, z_send.at[k - 1], z_recv.at[k - 1, i], (flip2, d))
                to_partner(ref, k, 0)
            elif kind == "x":
                ref = landed(block, q1, i, x_send.at[k - 1], x_recv.at[k - 1, i])
                if i in c_part:
                    m = CHUNKS + i - BY_X
                    push(ref, ref, z_send.at[k - 1], z_recv.at[k - 1, m], (flip2, d))
                to_partner(ref, k, 1 if i < SOON else 2)
            elif kind == "z":
                ref = landed(block, q2, i, z_send.at[k - 1], z_recv.at[k - 1, i])
                if i in b_part:
                    m = CHUNKS + i
                    push(ref, ref, x_send.at[k - 1], x_recv.at[k - 1, m], (flip1, d))
                to_partner(ref, k, 1 if i < SOON else 2)
            elif kind == "yd":
                m = CHUNKS + i - BY_X - BY_Z
                ref = landed(block, q3, i, y_send.at[k - 1], y_recv.at[k - 1, m])
                to_partner(ref, k, 2)
            elif kind == "xd":
                m = CHUNKS + i
                ref = landed(block, q3, i, x_send.at[k - 1], x_recv.at[k - 1, m])
                to_partner(ref, k, 2)
            else:
                m = CHUNKS + i - BY_X
                ref = landed(block, q3, i, z_send.at[k - 1], z_recv.at[k - 1, m])
                to_partner(ref, k, 2)

        return run

    plan = []
    unit = 11.2 / CHUNKS
    first_y, first_z, first_x = 1.9 + unit, 3.9 + 2 * unit, 4.4 + 2 * unit
    for k in range(1, groups):
        for i in range(CHUNKS):
            plan.append((first_y + unit * i, event("y", k, i)))
            later = 1.0
            plan.append((first_z + unit * i + later, event("z", k, i)))
            plan.append((first_x + unit * i + later, event("x", k, i)))
        for n, i in enumerate(a_part):
            plan.append((first_y + unit * (CHUNKS + n), event("yd", k, i)))
        for n, i in enumerate(c_part):
            plan.append((first_z + unit * (CHUNKS + n), event("zd", k, i)))
        for n, i in enumerate(b_part):
            plan.append((first_x + unit * (CHUNKS + n), event("xd", k, i)))

    step = 2 * LANES
    eye = (
        lax.broadcasted_iota(jnp.int32, (span, span), 0)
        == lax.broadcasted_iota(jnp.int32, (span, span), 1)
    ).astype(jnp.float32).astype(jnp.bfloat16)

    for i in range(4):
        loads[2 * i].wait()
        loads[2 * i + 1].wait()
        per = in_rows // step

        def turn(n, carry):
            at_row = pl.multiple_of(n * step, step)
            cut = pl.ds(at_row, step)
            glu = (
                lin_v[cut, :].astype(jnp.float32)
                * jax.nn.sigmoid(gate_v[cut, :].astype(jnp.float32))
            ).astype(jnp.bfloat16)
            turned = lax.dot_general(
                eye, glu, (((1,), (1,)), ((), ())), preferred_element_type=jnp.float32
            )
            for m in range(2):
                slab = turned[:, m * LANES : (m + 1) * LANES]
                gpad[2 * n + m, pl.ds(PAD, span), :] = slab
                edge_out[0, 2 * n + m] = slab[:PAD].astype(jnp.bfloat16)
                edge_out[1, 2 * n + m] = slab[span - PAD :].astype(jnp.bfloat16)
            return carry

        lax.fori_loop(i * per, (i + 1) * per, turn, 0)

    to_left = copy(edge_out.at[0], edge_in.at[0], halo_send.at[0], halo_recv.at[0], (s - 1, d))
    to_right = copy(edge_out.at[1], edge_in.at[1], halo_send.at[1], halo_recv.at[1], (s + 1, d))

    @pl.when(has_left)
    def _():
        to_left.start()

    @pl.when(has_right)
    def _():
        to_right.start()

    for c in small:
        c.wait()
    stat[0] = jnp.zeros((span, LANES), jnp.float32)

    own_loads[2].wait()
    own_loads[3].wait()
    push(wbuf.at[d], wbuf.at[d], own_d2d.at[0], own_d2d.at[1], partner)

    def halo():
        @pl.when(has_left)
        def _():
            to_right.wait_recv()
            gpad[:, 0:PAD, :] = edge_in[1].astype(jnp.float32)

        @pl.when(jnp.logical_not(has_left))
        def _():
            gpad[:, 0:PAD, :] = jnp.zeros((slabs, PAD, LANES), jnp.float32)

        @pl.when(has_right)
        def _():
            to_left.wait_recv()
            gpad[:, PAD + span :, :] = edge_in[0].astype(jnp.float32)

        @pl.when(jnp.logical_not(has_right))
        def _():
            gpad[:, PAD + span :, :] = jnp.zeros((slabs, PAD, LANES), jnp.float32)

    def taps_sum(n, base, count):
        lanes = pl.ds(pl.multiple_of(n * LANES, LANES), LANES)
        running = jnp.zeros((count, LANES), jnp.float32)
        for j in range(taps_n):
            weight = taps[pl.ds(j, 1), lanes]
            running = running + weight * gpad[n, pl.ds(base + (PAD - half + j), count), :]
        rounded = running.astype(jnp.bfloat16).astype(jnp.float32)
        at_token = pl.ds(pl.multiple_of(base, PAD), count)
        mixed[n, at_token, :] = rounded
        stat[0, at_token, :] += rounded

    inner = span - 2 * PAD
    tiles = next(m for m in range(2, inner) if inner % m == 0 and inner // m <= LANES and inner // m % PAD == 0)
    tile = inner // tiles

    def conv_slab(n, carry):
        def tokens(m, within):
            taps_sum(n, PAD + m * tile, tile)
            return within

        return lax.fori_loop(0, tiles, tokens, carry)

    def edges():
        def one(n, carry):
            def side(m, within):
                taps_sum(n, m * (span - PAD), PAD)
                return within

            return lax.fori_loop(0, 2, side, carry, unroll=True)

        lax.fori_loop(0, slabs, one, 0)

    parts = 8

    def conv(i):
        return lambda: lax.fori_loop(i * slabs // parts, (i + 1) * slabs // parts, conv_slab, 0)

    def norm():
        mean = jnp.sum(stat[0], axis=1, keepdims=True) * (1.0 / channels)
        stat[0] = jnp.broadcast_to(mean, (span, LANES))
        stat[1] = jnp.zeros((span, LANES), jnp.float32)

        def spread(n, carry):
            apart = mixed[n] - stat[0]
            stat[1] += apart * apart
            return carry

        lax.fori_loop(0, slabs, spread, 0)
        variance = jnp.sum(stat[1], axis=1, keepdims=True) * (1.0 / channels)
        stat[1] = jnp.broadcast_to(lax.rsqrt(variance + 1e-05), (span, LANES))

    def activate(h):
        def one(n, carry):
            lanes = pl.ds(pl.multiple_of(n * LANES, LANES), LANES)
            normed = (mixed[n] - stat[0]) * stat[1]
            normed = normed * gain[:, lanes] + shift[:, lanes]
            act[:, lanes] = (normed * jax.nn.sigmoid(normed)).astype(jnp.bfloat16)
            return carry

        lax.fori_loop(h * slabs // 2, (h + 1) * slabs // 2, one, 0)

    cols = min(width, 2 * LANES)

    halves = width // cols

    def sweep(block, body, first=0, count=halves):
        def columns(n, carry):
            at_col = pl.ds(pl.multiple_of(n * cols, cols), cols)
            at_out = pl.ds(pl.multiple_of(block * width + n * cols, cols), cols)
            body(at_col, at_out)
            return carry

        lax.fori_loop(first, first + count, columns, 0)

    def product(block, n):
        def body(at_col, at_out):
            out[:, at_out] = jnp.dot(
                act[...], wbuf[block, :, at_col], preferred_element_type=jnp.float32
            ).astype(out.dtype)

        sweep(block, body, n, 1)

    def slice_dot(block, p, at_col, low=0, high=CHUNKS):
        at_row = pl.ds(pl.multiple_of(p * piece + low * rows, LANES), (high - low) * rows)
        return jnp.dot(
            act[:, at_row], wbuf[block, at_row, at_col], preferred_element_type=jnp.float32
        )

    def stage(which, slot, block):
        def body(at_col, at_out):
            if which == 0:
                part[slot, :, at_col] = slice_dot(block, q, at_col)
            elif which == 1:
                total = part[slot, :, at_col] + slice_dot(block, q1, at_col, 0, SOON)
                part[slot, :, at_col] = total + slice_dot(block, q2, at_col, 0, SOON)
            else:
                total = part[slot, :, at_col] + slice_dot(block, q1, at_col, SOON)
                total = total + slice_dot(block, q2, at_col, SOON)
                out[:, at_out] = (total + slice_dot(block, q3, at_col)).astype(out.dtype)

        sweep(block, body)

    def near(k):
        return ((g + groups - k) % groups) * 2 + core

    def far(k):
        return ((g + groups - k) % groups) * 2 + 1 - core

    late = CHUNKS - SOON
    shares = (CHUNKS, 2 * SOON, 2 * late + CHUNKS)

    def stage_near(which, k):
        stage(which, 2 * k - 2, near(k))

    def stage_far(which, k):
        ref = wbuf.at[far(k), pl.ds(0, shares[which] * rows), :]
        copy(ref, ref, d_send.at[k - 1], d_recv.at[k - 1, which], partner).wait_recv()
        stage(which, 2 * k - 1, far(k))

    def take_other():
        copy(wbuf.at[other], wbuf.at[other], own_d2d.at[0], own_d2d.at[1], partner).wait_recv()

    for i in range(parts):
        plan.append((1.5 + 0.6 * i, conv(i)))
    plan.append((6.3, halo))
    plan.append((6.4, edges))
    plan.append((7.3, norm))
    plan.append((7.9, lambda: activate(0)))
    plan.append((8.3, lambda: activate(1)))
    for n in range(halves):
        plan.append((8.7 + 1.0 * n / halves, lambda n=n: product(d, n)))
        plan.append((9.8 + 1.0 * n / halves, lambda n=n: product(other, n)))
    plan.append((9.75, take_other))
    for k in range(1, groups):
        for which, when in ((0, 13.2), (1, 14.6)):
            plan.append((when, lambda k=k, which=which: stage_near(which, k)))
            plan.append((when + 1.2, lambda k=k, which=which: stage_far(which, k)))
    for _, action in sorted(plan, key=lambda entry: entry[0]):
        action()
    for k in range(1, groups):
        stage_near(2, k)
        stage_far(2, k)

    def sent(sem, size):
        ref = wbuf.at[d, pl.ds(0, size * rows), :]
        copy(ref, ref, sem, own_d2d.at[1], partner).wait_send()

    for k in range(1, groups):
        sent(y_send.at[k - 1], CHUNKS + BY_Y)
        sent(x_send.at[k - 1], CHUNKS + BY_X)
        sent(z_send.at[k - 1], CHUNKS + BY_Z)
        sent(d_send.at[k - 1], 4 * CHUNKS)
    sent(own_d2d.at[0], 4 * CHUNKS)

    @pl.when(has_left)
    def _():
        to_left.wait_send()

    @pl.when(has_right)
    def _():
        to_right.wait_send()


def solution(mesh):
    n_sp, n_dp = mesh.shape["sp"], mesh.shape["dp"]

    def per_device(lin_pre, gate_pre, w_depth, ln_gain, ln_shift, w_out):
        channels, span = lin_pre.shape
        width = w_out.shape[1]
        far = n_dp // 2 - 1
        slabs = channels // LANES
        dma = pltpu.SemaphoreType.DMA
        vmem = pl.BlockSpec(memory_space=pltpu.VMEM)
        hbm = pl.BlockSpec(memory_space=pl.ANY)
        return pl.pallas_call(
            functools.partial(kernel, n_sp, n_dp),
            out_shape=pltpu.VMEM((span, n_dp * width), jnp.bfloat16),
            in_specs=[hbm] * 6,
            out_specs=vmem,
            scratch_shapes=[
                pltpu.VMEM((channels, span), jnp.bfloat16),
                pltpu.VMEM((channels, span), jnp.bfloat16),
                pltpu.VMEM(w_depth.shape, jnp.float32),
                pltpu.VMEM((1, channels), jnp.float32),
                pltpu.VMEM((1, channels), jnp.float32),
                pltpu.VMEM((slabs, span + 2 * PAD, LANES), jnp.float32),
                pltpu.VMEM((slabs, span, LANES), jnp.float32),
                pltpu.VMEM((span, channels), jnp.bfloat16),
                pltpu.VMEM((n_dp, channels, width), jnp.bfloat16),
                pltpu.VMEM((2, span, LANES), jnp.float32),
                pltpu.VMEM((2 * far, span, width), jnp.float32),
                pltpu.VMEM((2, slabs, PAD, LANES), jnp.bfloat16),
                pltpu.VMEM((2, slabs, PAD, LANES), jnp.bfloat16),
                dma((2, 4)),
                dma((3,)),
                dma((5,)),
                dma((2,)),
                dma((2,)),
                dma((2,)),
                dma((far,)),
                dma((far, CHUNKS + BY_Y)),
                dma((far,)),
                dma((far, CHUNKS + BY_X)),
                dma((far,)),
                dma((far, CHUNKS + BY_Z)),
                dma((far,)),
                dma((far, 3)),
            ],
            compiler_params=pltpu.CompilerParams(
                collective_id=0, has_side_effects=True, vmem_limit_bytes=60 * 2**20
            ),
            name="conv_module",
        )(lin_pre, gate_pre, w_depth, ln_gain[None, :], ln_shift[None, :], w_out)

    in_specs = (P(None, ("dp", "sp")), P(None, ("dp", "sp")), P(), P(), P(), P(None, "dp"))
    out_specs = P(("dp", "sp"), None)
    return jax.shard_map(
        per_device, mesh=mesh, in_specs=in_specs, out_specs=out_specs, check_vma=False
    )
```
